32 devices in a mesh: rep: 2 (over x), fs: 8 (over z, y), tp: 2 (over core).
Axes of the slice: x: 2, y: 2, z: 4, core: 2. Of those that a mesh axis runs over, the one named last changes fastest.
Arguments:
- stream_in: bfloat16 [16, 768, 2048], P(('rep', 'fs'), None, 'tp'), may hold values from -6 to 6
- mix_gain: float32 [2048], replicated, may hold values from 0.1 to 1.9
- lin_weight: bfloat16 [2048, 2048], P('fs', 'tp'), may hold values from -0.125 to 0.125
- branch_weight: bfloat16 [2048, 2048], P('fs', 'tp'), may hold values from -0.125 to 0.125
- lin_taps: float32 [4, 2048], P(None, 'tp'), may hold values from -3 to 3
- rate_blocks: bfloat16 [16, 128, 128], P('tp'), may hold values from -0.5 to 0.5
- admit_blocks: bfloat16 [16, 128, 128], P('tp'), may hold values from -0.5 to 0.5
- decay_logit: float32 [2048], P('tp'), may hold values from 3.5 to 9
- mix_out_gain: float32 [2048], P('tp'), may hold values from 0.1 to 1.9
- out_weight: bfloat16 [2048, 2048], P('tp', 'fs'), may hold values from -0.125 to 0.125
- ffn_gain: float32 [2048], replicated, may hold values from 0.1 to 1.9
- gate_weight: bfloat16 [2048, 2816], P('fs', 'tp'), may hold values from -0.125 to 0.125
- up_weight: bfloat16 [2048, 2816], P('fs', 'tp'), may hold values from -0.125 to 0.125
- gate_taps: float32 [3, 2816], P(None, 'tp'), may hold values from -3 to 3
- up_taps: float32 [3, 2816], P(None, 'tp'), may hold values from -3 to 3
- down_weight: bfloat16 [2816, 2048], P('tp', 'fs'), may hold values from -0.109375 to 0.109375
Outputs:
- stream_out: bfloat16 [16, 768, 2048], P(('rep', 'fs'), None, 'tp')
The draws below stay inside these ranges and needn't reach their ends.
All inputs are finite; a program needn't handle non-finite values.
Results may differ from the reference program's by a relative error of at most 0.018.
Values may be sent and summed in bfloat16 or wider, within the bound.
No kernel may reach another device: no remote copies, remote signals or barrier semaphores. Data moves between devices by JAX's collectives and lax.ppermute only.
A program may use at most 128 MiB of HBM per device.

```python
import jax
import jax.numpy as jnp
from jax import lax

D = 2048
HD = 128
BLOCKS = 16
FF = 2816
LEN = 768
LRU = 2048
SEQS = 16
N_TP = 2


def steps_of(rng, dims, split, smallest, top_value):
    level = 1.0
    for axis_at, parts in split:
        heights = jax.random.uniform(jax.random.fold_in(jax.random.fold_in(rng, 6), axis_at), (parts,), jnp.float32, smallest / len(split), top_value / len(split))
        level = level * jnp.repeat(jnp.exp(heights), dims[axis_at] // parts).reshape((-1,) + (1,) * (len(dims) - 1 - axis_at))
    return level


def scatter_about(rng, dims, deviation, limit, cuts=(), held_as=jnp.bfloat16):
    level = steps_of(rng, dims, cuts, -0.22, 0.18) if cuts else 1.0
    array = jax.random.normal(rng, dims, jnp.float32) * deviation * level
    return jnp.minimum(jnp.maximum(array, -limit), limit).astype(held_as)


def setup_inputs(seed: int = 0) -> dict:
    streams_of = jax.random.split(jax.random.key(seed), 17)
    return {
        "stream_in": scatter_about(streams_of[0], (SEQS, LEN, D), 1.0, 6.0, ((0, 16), (2, 2))),
        "mix_gain": jnp.clip(1.0 + 0.18 * jax.random.normal(streams_of[1], (D,), jnp.float32), 0.1, 1.9),
        "lin_weight": scatter_about(streams_of[2], (D, LRU), D ** -0.5, 0.125, ((0, 8), (1, 2))),
        "branch_weight": scatter_about(streams_of[3], (D, LRU), D ** -0.5, 0.125, ((0, 8), (1, 2))),
        "lin_taps": scatter_about(streams_of[4], (4, LRU), 0.5, 3.0, ((1, 2),), jnp.float32),
        "rate_blocks": scatter_about(streams_of[5], (BLOCKS, HD, HD), HD ** -0.5, 0.5, ((0, 2),)),
        "admit_blocks": scatter_about(streams_of[6], (BLOCKS, HD, HD), HD ** -0.5, 0.5, ((0, 2),)),
        "decay_logit": jnp.clip(3.5 + 5.5 * jax.random.uniform(streams_of[7], (LRU,), jnp.float32) ** steps_of(streams_of[7], (LRU,), ((0, 2),), -0.2, 0.2), 3.5, 9.0),
        "mix_out_gain": jnp.clip(1.0 + 0.18 * jax.random.normal(streams_of[8], (LRU,), jnp.float32), 0.1, 1.9),
        "out_weight": scatter_about(streams_of[9], (LRU, D), LRU ** -0.5, 0.125, ((0, 2), (1, 8))),
        "ffn_gain": jnp.clip(1.0 + 0.18 * jax.random.normal(streams_of[10], (D,), jnp.float32), 0.1, 1.9),
        "gate_weight": scatter_about(streams_of[11], (D, FF), D ** -0.5, 0.125, ((0, 8), (1, 2))),
        "up_weight": scatter_about(streams_of[12], (D, FF), D ** -0.5, 0.125, ((0, 8), (1, 2))),
        "gate_taps": scatter_about(streams_of[13], (3, FF), 0.6, 3.0, ((1, 2),), jnp.float32),
        "up_taps": scatter_about(streams_of[14], (3, FF), 0.6, 3.0, ((1, 2),), jnp.float32),
        "down_weight": scatter_about(streams_of[15], (FF, D), FF ** -0.5, 0.109375, ((0, 2), (1, 8))),
    }


EPS = 1e-06
GATE_SCALE = 8.0

def norm_rows(values, scales):
    mean_sq = lax.optimization_barrier(jnp.mean(values * values, axis=-1, keepdims=True))
    return values * lax.rsqrt(mean_sq + EPS) * scales

def causal_filter(values, kernel):
    kernel_len = kernel.shape[0]
    seq_len = values.shape[0]
    padded = jnp.pad(values, ((kernel_len - 1, 0), (0, 0)))
    summed = padded[0:seq_len] * kernel[0]
    for offset in range(1, kernel_len):
        summed = summed + padded[offset:offset + seq_len] * kernel[offset]
    return summed

def chain_combine(earlier, later):
    return (earlier[0] * later[0], later[0] * earlier[1] + later[1])

def split_product(left, right):
    group = left.shape[1] // N_TP
    summed = jnp.zeros((left.shape[0], right.shape[1]), jnp.float32)
    for column_part in range(N_TP):
        partial_value = jnp.dot(left[:, column_part * group:(column_part + 1) * group], right[column_part * group:(column_part + 1) * group], preferred_element_type=jnp.float32)
        partial_value = lax.optimization_barrier(partial_value.astype(jnp.bfloat16))
        summed = summed + partial_value.astype(jnp.float32)
    return summed

def reference(stream_in, mix_gain, lin_weight, branch_weight, lin_taps, rate_blocks, admit_blocks, decay_logit, mix_out_gain, out_weight, ffn_gain, gate_weight, up_weight, gate_taps, up_taps, down_weight):

    def one_sequence(sequence):
        stream = sequence.astype(jnp.float32)
        normed = norm_rows(stream, mix_gain).astype(jnp.bfloat16)
        linear = jnp.dot(normed, lin_weight, preferred_element_type=jnp.float32).astype(jnp.bfloat16)
        branch = jnp.dot(normed, branch_weight, preferred_element_type=jnp.float32).astype(jnp.bfloat16)
        filtered = causal_filter(linear.astype(jnp.float32), lin_taps)
        blocks = filtered.astype(jnp.bfloat16).astype(jnp.float32).reshape(LEN, BLOCKS, HD)
        rate_gate = jax.nn.sigmoid(jnp.einsum('lbi,bij->lbj', blocks, rate_blocks.astype(jnp.float32)).reshape(LEN, BLOCKS * HD))
        admitted = jax.nn.sigmoid(jnp.einsum('lbi,bij->lbj', blocks, admit_blocks.astype(jnp.float32)).reshape(LEN, BLOCKS * HD))
        log_decay = -GATE_SCALE * rate_gate * jax.nn.softplus(-decay_logit)
        decay = jnp.exp(log_decay)
        driven = jnp.sqrt(-jnp.expm1(2.0 * log_decay)) * admitted * filtered
        _, states = lax.associative_scan(chain_combine, (decay, driven), axis=0)
        gated = (states * jax.nn.gelu(branch.astype(jnp.float32))).reshape(LEN, BLOCKS, HD)
        gated = gated * lax.rsqrt(lax.optimization_barrier(jnp.mean(gated * gated, axis=-1, keepdims=True)) + EPS)
        mixed = (gated.reshape(LEN, BLOCKS * HD) * mix_out_gain).astype(jnp.bfloat16)
        middle = (stream + split_product(mixed, out_weight)).astype(jnp.bfloat16)
        normed2 = norm_rows(middle.astype(jnp.float32), ffn_gain).astype(jnp.bfloat16)
        gate_pre = jnp.dot(normed2, gate_weight, preferred_element_type=jnp.float32).astype(jnp.bfloat16)
        up_pre = jnp.dot(normed2, up_weight, preferred_element_type=jnp.float32).astype(jnp.bfloat16)
        gate_conv = causal_filter(gate_pre.astype(jnp.float32), gate_taps)
        up_conv = causal_filter(up_pre.astype(jnp.float32), up_taps)
        hidden = (jax.nn.silu(gate_conv) * up_conv).astype(jnp.bfloat16)
        return (middle.astype(jnp.float32) + split_product(hidden, down_weight)).astype(jnp.bfloat16)
    return lax.map(one_sequence, stream_in)
```

```python
import functools

import jax
import jax.numpy as jnp
import numpy as np
from jax import lax
from jax.experimental import pallas as pl
from jax.experimental.pallas import tpu as pltpu
from jax.sharding import PartitionSpec as P

EPS = 1e-06
GATE_SCALE = 8.0
TILE = 16
F32 = jnp.float32
BF16 = jnp.bfloat16


VMEM = pl.BlockSpec(memory_space=pltpu.VMEM)
SMEM = pl.BlockSpec(memory_space=pltpu.SMEM)
HBM = pl.BlockSpec(memory_space=pltpu.HBM)


def row_block(length):
    return max(b for b in range(TILE, 257, TILE) if length % b == 0)


def fetch_rows(order_ref, pieces, wbuf, sems):
    rows = pieces[0].shape[0]
    copies = []
    for k, piece in enumerate(pieces):
        at = pl.multiple_of(order_ref[k] * rows, rows)
        copies.append(pltpu.make_async_copy(piece, wbuf.at[pl.ds(at, rows)], sems.at[k]))
    return copies


def fetch_blocks(order_ref, pieces, wbuf, sems):
    rows = pieces[0].shape[0]
    return [
        pltpu.make_async_copy(piece, wbuf.at[order_ref[k], pl.ds(0, rows)], sems.at[k])
        for k, piece in enumerate(pieces)
    ]


def norm_into(own_ref, peer_ref, gain_ref, normed_ref):
    length, half = own_ref.shape

    def step(i, _):
        at = pl.ds(pl.multiple_of(i * TILE, TILE), TILE)
        own = own_ref[at, :].astype(F32)
        peer = peer_ref[at, :].astype(F32)
        mean_sq = jnp.sum(own * own + peer * peer, axis=1, keepdims=True) * (0.5 / half)
        scale = lax.rsqrt(mean_sq + EPS)
        normed_ref[at, :half] = (own * scale * gain_ref[0:1, :]).astype(BF16)
        normed_ref[at, half:] = (peer * scale * gain_ref[1:2, :]).astype(BF16)
        return 0

    lax.fori_loop(0, length // TILE, step, 0, unroll=2)


def mix_kernel(n_pieces, order_ref, own_ref, peer_ref, gain_ref, taps_ref, gates_ref, slope_ref, out_gain_ref, *rest):
    pieces = rest[:n_pieces]
    mixed_ref, normed_ref, wbuf, linear_ref, branch_ref, filt_ref, gate_ref, sems = rest[n_pieces:]
    copies = fetch_rows(order_ref, pieces, wbuf, sems)
    for copy in copies:
        copy.start()
    length, width = mixed_ref.shape
    block_count, block, _ = gates_ref.shape
    norm_into(own_ref, peer_ref, gain_ref, normed_ref)
    for copy in copies:
        copy.wait()
    linear_ref[0:8, :] = jnp.zeros((8, width), F32)
    rows = row_block(length)

    def project(m, _):
        at = pl.multiple_of(m * rows, rows)
        both = jnp.dot(normed_ref[pl.ds(at, rows), :], wbuf[...], preferred_element_type=F32).astype(BF16)
        linear_ref[pl.ds(pl.multiple_of(at + 8, 8), rows), :] = both[:, :width].astype(F32)
        branch_ref[pl.ds(at, rows), :] = both[:, width:]
        return 0

    lax.fori_loop(0, length // rows, project, 0)

    def convolve(i, _):
        at = pl.multiple_of(i * TILE, TILE)
        window = linear_ref[pl.ds(at, TILE + 8), :]
        taps = taps_ref.shape[0]
        total = window[9 - taps : 9 - taps + TILE] * taps_ref[0:1, :]
        for j in range(1, taps):
            total = total + window[9 - taps + j : 9 - taps + j + TILE] * taps_ref[j : j + 1, :]
        filt_ref[pl.ds(at, TILE), :] = total
        return 0

    lax.fori_loop(0, length // TILE, convolve, 0)

    def gates(m, _):
        at = pl.ds(pl.multiple_of(m * rows, rows), rows)
        for b in range(block_count):
            piece = filt_ref[at, b * block : (b + 1) * block].astype(BF16)
            gate_ref[at, 2 * b * block : 2 * (b + 1) * block] = jnp.dot(
                piece, gates_ref[b], preferred_element_type=F32
            )
        return 0

    lax.fori_loop(0, length // rows, gates, 0)
    row = lax.broadcasted_iota(jnp.int32, (8, block), 0)

    def scan(i, carry):
        at = pl.ds(pl.multiple_of(i * TILE, TILE), TILE)
        ends = []
        for b in range(block_count):
            cols = slice(b * block, (b + 1) * block)
            filtered = filt_ref[at, cols]
            rate = jax.nn.sigmoid(gate_ref[at, 2 * b * block : (2 * b + 1) * block])
            admit = jax.nn.sigmoid(gate_ref[at, (2 * b + 1) * block : 2 * (b + 1) * block])
            log_decay = rate * slope_ref[0:1, cols]
            fall = 1.0 / 120 + log_decay * (1.0 / 720)
            for coef in (1.0 / 24, 1.0 / 6, 0.5, 1.0):
                fall = coef + log_decay * fall
            fall = log_decay * fall
            decay = 1.0 + fall
            driven = jnp.sqrt(-fall * (2.0 + fall)) * admit * filtered
            last = carry[b]
            states = []
            for part in range(TILE // 8):
                a = decay[part * 8 : part * 8 + 8]
                d = driven[part * 8 : part * 8 + 8]
                for shift in (1, 2, 4):
                    keep = row >= shift
                    d = jnp.where(keep, a * pltpu.roll(d, shift, 0) + d, d)
                    a = jnp.where(keep, a * pltpu.roll(a, shift, 0), a)
                h = a * last + d
                last = jnp.broadcast_to(h[7:8, :], (8, block))
                states.append(h)
            ends.append(last)
            x = branch_ref[at, cols].astype(F32)
            gelu = 0.5 * x * (1.0 + jnp.tanh(0.7978845608028654 * (x + 0.044715 * x * x * x)))
            gated = jnp.concatenate(states, axis=0) * gelu
            mean_sq = jnp.mean(gated * gated, axis=1, keepdims=True)
            mixed_ref[at, cols] = (gated * lax.rsqrt(mean_sq + EPS) * out_gain_ref[0:1, cols]).astype(BF16)
        return tuple(ends)

    zero = jnp.zeros((8, block), F32)
    lax.fori_loop(0, length // TILE, scan, (zero,) * block_count)


def ffn_kernel(n_pieces, order_ref, own_ref, peer_ref, gain_ref, taps_ref, *rest):
    pieces = rest[:n_pieces]
    hidden_ref, normed_ref, wbuf, pre_ref, sems = rest[n_pieces:]
    copies = fetch_rows(order_ref, pieces, wbuf, sems)
    for copy in copies:
        copy.start()
    length = own_ref.shape[0]
    width = wbuf.shape[1]
    taps = taps_ref.shape[0]
    whole = width // 256
    norm_into(own_ref, peer_ref, gain_ref, normed_ref)
    for copy in copies:
        copy.wait()
    rows = row_block(length)
    pre_ref[0:8, :] = jnp.zeros((8, width), F32)
    low = lax.broadcasted_iota(jnp.int32, (TILE, 128), 1) < 64

    def project(m, _):
        at = pl.multiple_of(m * rows, rows)
        pre = jnp.dot(normed_ref[pl.ds(at, rows), :], wbuf[...], preferred_element_type=F32)
        pre_ref[8 : 8 + rows, :] = pre.astype(BF16).astype(F32)

        def activate(i, _):
            r = pl.multiple_of(i * TILE, TILE)

            def conv(col):
                cols = slice(col, col + 128)
                window = pre_ref[pl.ds(r, TILE + 8), cols]
                total = window[9 - taps : 9 - taps + TILE] * taps_ref[0:1, cols]
                for j in range(1, taps):
                    total = total + window[9 - taps + j : 9 - taps + j + TILE] * taps_ref[j : j + 1, cols]
                return total

            out = pl.ds(pl.multiple_of(at + r, TILE), TILE)
            for b in range(whole):
                hidden = jax.nn.silu(conv(b * 128)) * conv((whole + b) * 128)
                hidden_ref[out, b * 128 : (b + 1) * 128] = hidden.astype(BF16)
            if width % 256:
                both = conv(2 * whole * 128)
                hidden = jnp.where(low, jax.nn.silu(both) * pltpu.roll(both, 64, 1), 0.0)
                hidden_ref[out, whole * 128 : (whole + 1) * 128] = hidden.astype(BF16)
            return 0

        lax.fori_loop(0, rows // TILE, activate, 0)
        pre_ref[0:8, :] = pre_ref[rows : rows + 8, :]
        return 0

    lax.fori_loop(0, length // rows, project, 0)


def out_kernel(n_pieces, order_ref, left_ref, *rest):
    pieces = rest[:n_pieces]
    keep_ref, send_ref, wbuf, sems = rest[n_pieces:]
    copies = fetch_blocks(order_ref, pieces, wbuf, sems)
    for copy in copies:
        copy.start()
    depth = pieces[0].shape[0]
    blocks, padded, width = wbuf.shape
    if padded > depth:
        wbuf[:, depth:, :] = jnp.zeros((blocks, padded - depth, width), BF16)
    length = left_ref.shape[0]
    rows = row_block(length)
    for copy in copies:
        copy.wait()

    def step(m, _):
        at = pl.ds(pl.multiple_of(m * rows, rows), rows)
        left = left_ref[at, :]
        for j in range(blocks):
            part = jnp.dot(left, wbuf[j], preferred_element_type=F32).astype(BF16)
            target = keep_ref if j < blocks // 2 else send_ref
            col = (j % (blocks // 2)) * width
            target[at, col : col + width] = part
        return 0

    lax.fori_loop(0, length // rows, step, 0)


def call(kernel, name, outs, scratch, limit_mib, flops, operands, pieces):
    specs = [SMEM] + [VMEM] * (len(operands) - 1) + [HBM] * len(pieces)
    return pl.pallas_call(
        functools.partial(kernel, len(pieces)),
        out_shape=outs,
        in_specs=specs,
        out_specs=jax.tree.map(lambda _: VMEM, outs),
        scratch_shapes=scratch + [pltpu.SemaphoreType.DMA((len(pieces),))],
        compiler_params=pltpu.CompilerParams(vmem_limit_bytes=limit_mib * 1024 * 1024),
        cost_estimate=pl.CostEstimate(flops=flops, bytes_accessed=2**22, transcendentals=0),
        name=name,
    )(*operands, *pieces)


def line_ring(n):
    return [0] + list(range(1, n, 2)) + [i for i in range(n - 1, 0, -1) if i % 2 == 0]


def piece_table(n_fs):
    outer = n_fs // 2
    ring = line_ring(outer)
    table = np.zeros((n_fs, 2, n_fs), np.int32)
    for f in range(n_fs):
        z, y = divmod(f, 2)
        found = [ring[(ring.index(z) - k) % outer] for k in range(outer)]
        owners = [q * 2 + y for q in found] + [q * 2 + 1 - y for q in found]
        for c in range(2):
            for k, owner in enumerate(owners):
                half, inside = divmod(owner, n_fs // 2)
                table[f, c, k] = (half ^ c) * (n_fs // 2) + inside
    return table.reshape(n_fs * 2, n_fs)


def local(
    n_fs,
    stream_in,
    mix_gain,
    lin_weight,
    branch_weight,
    lin_taps,
    rate_blocks,
    admit_blocks,
    decay_logit,
    mix_out_gain,
    out_weight,
    ffn_gain,
    gate_weight,
    up_weight,
    gate_taps,
    up_taps,
    down_weight,
):
    outer = n_fs // 2
    ring = line_ring(outer)
    ring_pairs = [
        (ring[p] * 2 + y, ring[(p + 1) % outer] * 2 + y) for p in range(outer) for y in range(2)
    ]
    swap_pairs = [(f, f ^ 1) for f in range(n_fs)]
    flip = [(0, 1), (1, 0)]

    def across(value):
        return lax.ppermute(value, "rep", flip)

    def partner(value):
        return lax.ppermute(value, "tp", flip)

    def gather_z_first(own):
        found = [own]
        for _ in range(outer - 1):
            found.append(lax.ppermute(found[-1], "fs", ring_pairs))
        return found + [lax.ppermute(q, "fs", swap_pairs) for q in found]

    x = lax.axis_index("rep")
    c = lax.axis_index("tp")
    f = lax.axis_index("fs")
    order = jnp.asarray(piece_table(n_fs))[f * 2 + c]

    def half_of(value, axis):
        size = value.shape[axis] // 2
        return lax.dynamic_slice_in_dim(value, x * size, size, axis)

    own = stream_in[0]
    length, half = own.shape
    channels = lin_weight.shape[1] // 2
    units = gate_weight.shape[1] // 2
    full = units // 128 * 128

    def interleave(gate, up):
        gate, up = half_of(gate, 1), half_of(up, 1)
        return jnp.concatenate([gate[:, :full], up[:, :full], gate[:, full:], up[:, full:]], axis=1)

    mix_pieces = gather_z_first(jnp.concatenate([half_of(lin_weight, 1), half_of(branch_weight, 1)], axis=1))
    other = across(own)
    own_peer = partner(own)
    other_peer = partner(other)
    out_pieces = gather_z_first(half_of(out_weight, 0))
    ffn_pieces = gather_z_first(interleave(gate_weight, up_weight))
    down_pieces = gather_z_first(half_of(down_weight, 0))

    gates = jnp.concatenate([half_of(rate_blocks, 0), half_of(admit_blocks, 0)], axis=2)
    slope = -GATE_SCALE * jax.nn.softplus(-half_of(decay_logit, 0))[None]
    out_gain = half_of(mix_out_gain, 0)[None]
    taps = half_of(lin_taps, 1)
    gain = jnp.where(c == 0, mix_gain.reshape(2, half), mix_gain.reshape(2, half)[::-1])
    gain2 = jnp.where(c == 0, ffn_gain.reshape(2, half), ffn_gain.reshape(2, half)[::-1])
    ffn_taps = interleave(gate_taps, up_taps)
    padded_units = -(-units // 128) * 128

    def mix(stream, peer):
        return call(
            mix_kernel,
            "mix",
            jax.ShapeDtypeStruct((length, channels), BF16),
            [
                pltpu.VMEM((length, 2 * half), BF16),
                pltpu.VMEM((2 * half, 2 * channels), BF16),
                pltpu.VMEM((length + 8, channels), F32),
                pltpu.VMEM((length, channels), BF16),
                pltpu.VMEM((length, channels), F32),
                pltpu.VMEM((length, 2 * channels), F32),
            ],
            28,
            length * 2 * half * 2 * channels * 2,
            [order, stream, peer, gain, taps, gates, slope, out_gain],
            mix_pieces,
        )

    def project(left, pieces, depth, name):
        sums = jax.ShapeDtypeStruct((length, half), BF16)
        return call(
            out_kernel,
            name,
            (sums, sums),
            [pltpu.VMEM((n_fs, depth, pieces[0].shape[1]), BF16)],
            16,
            length * depth * 2 * half * 2,
            [order, left],
            pieces,
        )

    def ffn(stream, peer):
        width = 2 * units
        return call(
            ffn_kernel,
            "ffn",
            jax.ShapeDtypeStruct((length, padded_units), BF16),
            [
                pltpu.VMEM((length, 2 * half), BF16),
                pltpu.VMEM((2 * half, width), BF16),
                pltpu.VMEM((row_block(length) + 8, width), F32),
            ],
            28,
            length * 2 * half * width * 2,
            [order, stream, peer, gain2, ffn_taps],
            ffn_pieces,
        )

    def add(*terms):
        return functools.reduce(lambda p, q: p + q, [t.astype(F32) for t in terms]).astype(BF16)

    mixed_other = mix(other, other_peer)
    keep_other, send_other = project(mixed_other, out_pieces, channels, "out")
    sent = across(add(keep_other, partner(send_other)))
    mixed_own = mix(own, own_peer)
    keep_own, send_own = project(mixed_own, out_pieces, channels, "out")
    middle = add(own, keep_own, partner(send_own), sent)

    middle_other = across(middle)
    middle_peer = partner(middle)
    hidden_own = ffn(middle, middle_peer)
    hidden_other = ffn(middle_other, partner(middle_other))
    keep_other, send_other = project(hidden_other, down_pieces, padded_units, "down")
    sent = across(add(keep_other, partner(send_other)))
    keep_own, send_own = project(hidden_own, down_pieces, padded_units, "down")
    return add(middle, keep_own, partner(send_own), sent)[None]


def solution(mesh):
    placed = (
        P(("rep", "fs"), None, "tp"),
        P(),
        P("fs", "tp"),
        P("fs", "tp"),
        P(None, "tp"),
        P("tp", None, None),
        P("tp", None, None),
        P("tp"),
        P("tp"),
        P("tp", "fs"),
        P(),
        P("fs", "tp"),
        P("fs", "tp"),
        P(None, "tp"),
        P(None, "tp"),
        P("tp", "fs"),
    )
    return jax.shard_map(
        functools.partial(local, mesh.shape["fs"]),
        mesh=mesh,
        in_specs=placed,
        out_specs=P(("rep", "fs"), None, "tp"),
        check_vma=False,
    )
```

```python
import functools

import jax
import jax.numpy as jnp
import numpy as np
from jax import lax
from jax.experimental import pallas as pl
from jax.experimental.pallas import tpu as pltpu
from jax.sharding import PartitionSpec as P


EPS = 1e-06
GATE_SCALE = 8.0
TILE = 16
PARTS = 2
BLOCK_ROWS = 768
NORM_UNROLL = 8
SCAN_UNROLL = 3
ACT_UNROLL = 4
F32 = jnp.float32
BF16 = jnp.bfloat16


VMEM = pl.BlockSpec(memory_space=pltpu.VMEM)
SMEM = pl.BlockSpec(memory_space=pltpu.SMEM)
HBM = pl.BlockSpec(memory_space=pltpu.HBM)


def row_block(length):
    return max(b for b in range(TILE, BLOCK_ROWS + 1, TILE) if length % b == 0)


def fetch_rows(order_ref, pieces, wbuf, sems):
    rows = pieces[0].shape[0]
    copies = []
    for k, piece in enumerate(pieces):
        at = pl.multiple_of(order_ref[k] * rows, rows)
        copies.append(pltpu.make_async_copy(piece, wbuf.at[pl.ds(at, rows)], sems.at[k]))
    return copies


def fetch_blocks(order_ref, pieces, wbuf, sems):
    blocks = wbuf.shape[0]
    per = blocks // len(pieces)
    rows = pieces[0].shape[0] // per
    copies = []
    for k in range(blocks):
        source = pieces[k % len(pieces)].at[pl.ds(k // len(pieces) * rows, rows)]
        copies.append(pltpu.make_async_copy(source, wbuf.at[order_ref[k], pl.ds(0, rows)], sems.at[k]))
    return copies


def norm_into(own_ref, peer_ref, gain_ref, normed_ref):
    length, half = own_ref.shape

    def step(i, _):
        at = pl.ds(pl.multiple_of(i * TILE, TILE), TILE)
        own = own_ref[at, :].astype(F32)
        peer = peer_ref[at, :].astype(F32)
        mean_sq = jnp.sum(own * own + peer * peer, axis=1, keepdims=True) * (0.5 / half)
        scale = lax.rsqrt(mean_sq + EPS)
        normed_ref[at, :half] = (own * scale * gain_ref[0:1, :]).astype(BF16)
        normed_ref[at, half:] = (peer * scale * gain_ref[1:2, :]).astype(BF16)
        return 0

    lax.fori_loop(0, length // TILE, step, 0, unroll=NORM_UNROLL)


def fetch_streams(sources, buffers, sems, first):
    copies = []
    for k, (source, buffer) in enumerate(zip(sources, buffers)):
        rows = buffer.shape[0]
        part = source.at[pl.ds(source.shape[0] - rows, rows)]
        copies.append(pltpu.make_async_copy(part, buffer, sems.at[first + k]))
    return copies


def mix_kernel(n_pieces, order_ref, gain_ref, taps_ref, gates_ref, slope_ref, out_gain_ref, *rest):
    n_pieces -= 2
    streams, pieces = rest[:2], rest[2 : n_pieces + 2]
    mixed_ref, own_ref, peer_ref, normed_ref, wbuf, linear_ref, branch_ref, filt_ref, gate_ref, sems = rest[
        n_pieces + 2 :
    ]
    stream_copies = fetch_streams(streams, (own_ref, peer_ref), sems, n_pieces)
    copies = fetch_rows(order_ref, pieces, wbuf, sems)
    for copy in stream_copies + copies:
        copy.start()
    for copy in stream_copies:
        copy.wait()
    length, width = mixed_ref.shape
    block_count, block, _ = gates_ref.shape
    taps = taps_ref.shape[0]
    norm_into(own_ref, peer_ref, gain_ref, normed_ref)
    for copy in copies:
        copy.wait()
    linear_ref[0:8, :] = jnp.zeros((8, width), F32)
    rows = row_block(length)

    def project(m, _):
        at = pl.multiple_of(m * rows, rows)
        both = jnp.dot(normed_ref[pl.ds(at, rows), :], wbuf[...], preferred_element_type=F32).astype(BF16)
        linear_ref[pl.ds(pl.multiple_of(at + 8, 8), rows), :] = both[:, :width].astype(F32)
        branch_ref[pl.ds(at, rows), :] = both[:, width:]
        return 0

    lax.fori_loop(0, length // rows, project, 0)

    def convolve(i, _):
        at = pl.multiple_of(i * TILE, TILE)
        window = linear_ref[pl.ds(at, TILE + 8), :]
        total = window[9 - taps : 9 - taps + TILE] * taps_ref[0:1, :]
        for j in range(1, taps):
            total = total + window[9 - taps + j : 9 - taps + j + TILE] * taps_ref[j : j + 1, :]
        filt_ref[pl.ds(at, TILE), :] = total
        return 0

    lax.fori_loop(0, length // TILE, convolve, 0, unroll=2)

    def gates(m, _):
        at = pl.ds(pl.multiple_of(m * rows, rows), rows)
        for b in range(block_count):
            piece = filt_ref[at, b * block : (b + 1) * block].astype(BF16)
            gate_ref[at, 2 * b * block : 2 * (b + 1) * block] = jnp.dot(
                piece, gates_ref[b], preferred_element_type=F32
            )
        return 0

    lax.fori_loop(0, length // rows, gates, 0)
    row = lax.broadcasted_iota(jnp.int32, (8, block), 0)

    def scan(i, carry):
        at = pl.ds(pl.multiple_of(i * TILE, TILE), TILE)
        ends = []
        for b in range(block_count):
            cols = slice(b * block, (b + 1) * block)
            filtered = filt_ref[at, cols]
            rate = jax.nn.sigmoid(gate_ref[at, 2 * b * block : (2 * b + 1) * block])
            admit = jax.nn.sigmoid(gate_ref[at, (2 * b + 1) * block : 2 * (b + 1) * block])
            log_decay = rate * slope_ref[0:1, cols]
            fall = 1.0 / 120 + log_decay * (1.0 / 720)
            for coef in (1.0 / 24, 1.0 / 6, 0.5, 1.0):
                fall = coef + log_decay * fall
            fall = log_decay * fall
            decay = 1.0 + fall
            driven = jnp.sqrt(-fall * (2.0 + fall)) * admit * filtered
            last = carry[b]
            states = []
            for part in range(TILE // 8):
                a = decay[part * 8 : part * 8 + 8]
                d = driven[part * 8 : part * 8 + 8]
                for shift in (1, 2, 4):
                    keep = row >= shift
                    d = jnp.where(keep, a * pltpu.roll(d, shift, 0) + d, d)
                    a = jnp.where(keep, a * pltpu.roll(a, shift, 0), a)
                h = a * last + d
                last = jnp.broadcast_to(h[7:8, :], (8, block))
                states.append(h)
            ends.append(last)
            x = branch_ref[at, cols].astype(F32)
            gelu = 0.5 * x * (1.0 + jnp.tanh(0.7978845608028654 * (x + 0.044715 * x * x * x)))
            gated = jnp.concatenate(states, axis=0) * gelu
            mean_sq = jnp.mean(gated * gated, axis=1, keepdims=True)
            mixed_ref[at, cols] = (gated * lax.rsqrt(mean_sq + EPS) * out_gain_ref[0:1, cols]).astype(BF16)
        return tuple(ends)

    zero = jnp.zeros((8, block), F32)
    lax.fori_loop(0, length // TILE, scan, (zero,) * block_count, unroll=SCAN_UNROLL)


def add_kernel(starts, *refs):
    out_ref = refs[-1]

    def step(i, _):
        at = pl.multiple_of(i * TILE, TILE)
        total = None
        for start, ref in zip(starts, refs):
            term = ref[pl.ds(pl.multiple_of(start + at, TILE), TILE), :].astype(F32)
            total = term if total is None else total + term
        out_ref[pl.ds(at, TILE), :] = total.astype(BF16)
        return 0

    lax.fori_loop(0, out_ref.shape[0] // TILE, step, 0, unroll=2)


def ffn_kernel(halo, chunks, n_pieces, order_ref, gain_ref, taps_ref, *rest):
    if halo:
        before_ref, rest = rest[0], rest[1:]
    n_streams = 2 * chunks
    n_pieces -= n_streams
    streams, pieces = rest[:n_streams], rest[n_streams : n_pieces + n_streams]
    hidden_ref, after_ref, own_ref, peer_ref, normed_ref, wbuf, pre_ref, sems = rest[n_pieces + n_streams :]
    buffers = []
    for k, stream in enumerate(streams):
        rows = stream.shape[0]
        buffers.append((own_ref, peer_ref)[k // chunks].at[pl.ds(k % chunks * rows, rows)])
    stream_copies = fetch_streams(streams, buffers, sems, n_pieces)
    copies = fetch_rows(order_ref, pieces, wbuf, sems)
    for copy in stream_copies + copies:
        copy.start()
    for copy in stream_copies:
        copy.wait()
    length = own_ref.shape[0]
    width = wbuf.shape[1]
    taps = taps_ref.shape[0]
    whole = width // 256
    norm_into(own_ref, peer_ref, gain_ref, normed_ref)
    for copy in copies:
        copy.wait()
    rows = row_block(length)
    pre_ref[0:8, :] = before_ref[...] if halo else jnp.zeros((8, width), F32)
    low = lax.broadcasted_iota(jnp.int32, (TILE, 128), 1) < 64

    def project(m, _):
        at = pl.multiple_of(m * rows, rows)
        pre = jnp.dot(normed_ref[pl.ds(at, rows), :], wbuf[...], preferred_element_type=F32)
        pre_ref[8 : 8 + rows, :] = pre.astype(BF16).astype(F32)

        def activate(i, _):
            r = pl.multiple_of(i * TILE, TILE)

            def conv(col):
                cols = slice(col, col + 128)
                window = pre_ref[pl.ds(r, TILE + 8), cols]
                total = window[9 - taps : 9 - taps + TILE] * taps_ref[0:1, cols]
                for j in range(1, taps):
                    total = total + window[9 - taps + j : 9 - taps + j + TILE] * taps_ref[j : j + 1, cols]
                return total

            out = pl.ds(pl.multiple_of(at + r, TILE), TILE)
            for b in range(whole):
                hidden = jax.nn.silu(conv(b * 128)) * conv((whole + b) * 128)
                hidden_ref[out, b * 128 : (b + 1) * 128] = hidden.astype(BF16)
            if width % 256:
                both = conv(2 * whole * 128)
                hidden = jnp.where(low, jax.nn.silu(both) * pltpu.roll(both, 64, 1), 0.0)
                hidden_ref[out, whole * 128 : (whole + 1) * 128] = hidden.astype(BF16)
            return 0

        lax.fori_loop(0, rows // TILE, activate, 0, unroll=ACT_UNROLL)
        pre_ref[0:8, :] = pre_ref[rows : rows + 8, :]
        return 0

    lax.fori_loop(0, length // rows, project, 0)
    after_ref[...] = pre_ref[0:8, :]


def out_kernel(parts, n_pieces, order_ref, left_ref, *rest):
    pieces = rest[:n_pieces]
    keeps, sends = rest[n_pieces : n_pieces + parts], rest[n_pieces + parts : n_pieces + 2 * parts]
    wbuf, sems = rest[n_pieces + 2 * parts :]
    copies = fetch_blocks(order_ref, pieces, wbuf, sems)
    for copy in copies:
        copy.start()
    blocks, padded, width = wbuf.shape
    depth = pieces[0].shape[0] * len(pieces) // blocks
    if padded > depth:
        wbuf[:, depth:, :] = jnp.zeros((blocks, padded - depth, width), BF16)
    length = keeps[0].shape[0]
    rows = row_block(length)
    for copy in copies:
        copy.wait()
    for part in range(parts):

        def step(m, _):
            at = pl.multiple_of(m * rows, rows)
            left = left_ref[pl.ds(pl.multiple_of(part * length + at, rows), rows), :]
            for j in range(blocks):
                total = jnp.dot(left, wbuf[j], preferred_element_type=F32).astype(BF16)
                target = (keeps if j < blocks // 2 else sends)[part]
                col = (j % (blocks // 2)) * width
                target[pl.ds(at, rows), col : col + width] = total
            return 0

        lax.fori_loop(0, length // rows, step, 0)


def call(kernel, outs, scratch, limit_mib, flops, operands, pieces, copies=None):
    specs = [SMEM] + [VMEM] * (len(operands) - 1) + [HBM] * len(pieces)
    return pl.pallas_call(
        functools.partial(kernel, len(pieces)),
        out_shape=outs,
        in_specs=specs,
        out_specs=jax.tree.map(lambda _: VMEM, outs),
        scratch_shapes=scratch + [pltpu.SemaphoreType.DMA((copies or len(pieces),))],
        compiler_params=pltpu.CompilerParams(vmem_limit_bytes=limit_mib * 1024 * 1024),
        cost_estimate=pl.CostEstimate(flops=flops, bytes_accessed=2**22, transcendentals=0),
    )(*operands, *pieces)


def line_ring(n):
    return [0] + list(range(1, n, 2)) + [i for i in range(n - 1, 0, -1) if i % 2 == 0]


def piece_table(n_fs):
    outer = n_fs // 2
    ring = line_ring(outer)
    table = np.zeros((n_fs, 2, n_fs), np.int32)
    for f in range(n_fs):
        z, y = divmod(f, 2)
        found = [ring[(ring.index(z) - k) % outer] for k in range(outer)]
        owners = [q * 2 + y for q in found] + [q * 2 + 1 - y for q in found]
        for c in range(2):
            for k, owner in enumerate(owners):
                half, inside = divmod(owner, n_fs // 2)
                table[f, c, k] = (half ^ c) * (n_fs // 2) + inside
    return table.reshape(n_fs * 2, n_fs)


def local(
    n_fs,
    stream_in,
    mix_gain,
    lin_weight,
    branch_weight,
    lin_taps,
    rate_blocks,
    admit_blocks,
    decay_logit,
    mix_out_gain,
    out_weight,
    ffn_gain,
    gate_weight,
    up_weight,
    gate_taps,
    up_taps,
    down_weight,
):
    outer = n_fs // 2
    ring = line_ring(outer)
    ring_pairs = [
        (ring[p] * 2 + y, ring[(p + 1) % outer] * 2 + y) for p in range(outer) for y in range(2)
    ]
    back_pairs = [(b, a) for a, b in ring_pairs]
    swap_pairs = [(f, f ^ 1) for f in range(n_fs)]
    flip = [(0, 1), (1, 0)]

    def across(value):
        return lax.ppermute(value, "rep", flip)

    def partner(value):
        return lax.ppermute(value, "tp", flip)

    def around(own, ahead=outer // 2):
        found = {0: own}
        for k in range(1, ahead + 1):
            found[k] = lax.ppermute(found[k - 1], "fs", ring_pairs)
        for k in range(outer - 1, ahead, -1):
            found[k] = lax.ppermute(found[(k + 1) % outer], "fs", back_pairs)
        return [found[k] for k in range(outer)]

    def gather_z_first(own, ahead=outer // 2):
        found = around(own, ahead)
        return found + [lax.ppermute(q, "fs", swap_pairs) for q in found]

    def gather_y_first(own):
        return around(jnp.concatenate([own, lax.ppermute(own, "fs", swap_pairs)], axis=0))

    x = lax.axis_index("rep")
    c = lax.axis_index("tp")
    f = lax.axis_index("fs")
    order = jnp.asarray(piece_table(n_fs))[f * 2 + c]

    def half_of(value, axis):
        size = value.shape[axis] // 2
        return lax.dynamic_slice_in_dim(value, x * size, size, axis)

    own = stream_in[0]
    length, half = own.shape
    part = length // PARTS
    channels = lin_weight.shape[1] // 2
    units = gate_weight.shape[1] // 2
    full = units // 128 * 128

    def interleave(gate, up):
        gate, up = half_of(gate, 1), half_of(up, 1)
        return jnp.concatenate([gate[:, :full], up[:, :full], gate[:, full:], up[:, full:]], axis=1)

    both = jnp.concatenate([half_of(lin_weight, 1), half_of(branch_weight, 1)], axis=1)
    mix_pieces = gather_z_first(both, outer - 1)
    other = across(own)
    own_peer = partner(own)
    other_peer = partner(other)
    out_pieces = gather_z_first(half_of(out_weight, 0))
    ffn_pieces = gather_z_first(interleave(gate_weight, up_weight))
    down_pieces = gather_y_first(half_of(down_weight, 0))

    gates = jnp.concatenate([half_of(rate_blocks, 0), half_of(admit_blocks, 0)], axis=2)
    slope = -GATE_SCALE * jax.nn.softplus(-half_of(decay_logit, 0))[None]
    out_gain = half_of(mix_out_gain, 0)[None]
    taps = half_of(lin_taps, 1)
    gain = jnp.where(c == 0, mix_gain.reshape(2, half), mix_gain.reshape(2, half)[::-1])
    gain2 = jnp.where(c == 0, ffn_gain.reshape(2, half), ffn_gain.reshape(2, half)[::-1])
    ffn_taps = interleave(gate_taps, up_taps)
    padded_units = -(-units // 128) * 128

    def mix(stream, peer):
        return call(
            mix_kernel,
            jax.ShapeDtypeStruct((length, channels), BF16),
            [
                pltpu.VMEM((length, half), BF16),
                pltpu.VMEM((length, half), BF16),
                pltpu.VMEM((length, 2 * half), BF16),
                pltpu.VMEM((2 * half, 2 * channels), BF16),
                pltpu.VMEM((length + 8, channels), F32),
                pltpu.VMEM((length, channels), BF16),
                pltpu.VMEM((length, channels), F32),
                pltpu.VMEM((length, 2 * channels), F32),
            ],
            30,
            length * 2 * half * 2 * channels * 2,
            [order, gain, taps, gates, slope, out_gain],
            [stream, peer] + mix_pieces,
        )

    def project(left, pieces):
        rows, depth = left.shape
        parts = rows // part
        sums = [jax.ShapeDtypeStruct((part, half), BF16)] * (2 * parts)
        outs = call(
            functools.partial(out_kernel, parts),
            sums,
            [pltpu.VMEM((n_fs, depth, pieces[0].shape[1]), BF16)],
            16,
            rows * depth * 2 * half * 2,
            [order, left],
            pieces,
            n_fs,
        )
        return outs[:parts], outs[parts:]

    def ffn(owns, peers, before):
        width = 2 * units
        rows = len(owns) * part
        halo = [] if before is None else [before]
        return call(
            functools.partial(ffn_kernel, bool(halo), len(owns)),
            (jax.ShapeDtypeStruct((rows, padded_units), BF16), jax.ShapeDtypeStruct((8, width), F32)),
            [
                pltpu.VMEM((rows, half), BF16),
                pltpu.VMEM((rows, half), BF16),
                pltpu.VMEM((rows, 2 * half), BF16),
                pltpu.VMEM((2 * half, width), BF16),
                pltpu.VMEM((row_block(rows) + 8, width), F32),
            ],
            28,
            rows * 2 * half * width * 2,
            [order, gain2, ffn_taps] + halo,
            owns + peers + ffn_pieces,
        )

    def add(*terms):
        starts = [t[1] if isinstance(t, tuple) else 0 for t in terms]
        arrays = [t[0] if isinstance(t, tuple) else t for t in terms]
        return pl.pallas_call(
            functools.partial(add_kernel, starts),
            out_shape=jax.ShapeDtypeStruct((part, half), BF16),
            in_specs=[VMEM] * len(arrays),
            out_specs=VMEM,
            compiler_params=pltpu.CompilerParams(vmem_limit_bytes=12 * 1024 * 1024),
            cost_estimate=pl.CostEstimate(flops=part * half * len(arrays), bytes_accessed=2**21, transcendentals=0),
        )(*arrays)

    mixed_other = mix(other, other_peer)
    keep_other, send_other = project(mixed_other, out_pieces)
    sent = []
    for i in range(PARTS):
        value = add(keep_other[i], partner(send_other[i]))
        sent.append(across(value))
    mixed_own = mix(own, own_peer)
    keep_own, send_own = project(mixed_own, out_pieces)
    middle, middle_peer, middle_other = [], [], []
    for i in range(PARTS):
        value = add((own, i * part), keep_own[i], partner(send_own[i]), sent[i])
        middle.append(value)
        middle_other.append(across(value))
        middle_peer.append(partner(value))
    other_middle_peer = [partner(value) for value in middle_other]

    tail, sent = None, []
    for i in range(PARTS):
        hidden, tail = ffn([middle_other[i]], [other_middle_peer[i]], tail)
        keep, send = project(hidden, down_pieces)
        sent.append(across(add(keep[0], partner(send[0]))))
    hidden, _ = ffn(middle, middle_peer, None)
    keeps, sends = project(hidden, down_pieces)
    result = []
    for i in range(PARTS):
        terms = [middle[i], keeps[i], partner(sends[i]), sent[i]]
        result.append(functools.reduce(jnp.add, [t.astype(F32) for t in terms]).astype(BF16))
    return jnp.concatenate(result, axis=0)[None]


def solution(mesh):
    placed = (
        P(("rep", "fs"), None, "tp"),
        P(),
        P("fs", "tp"),
        P("fs", "tp"),
        P(None, "tp"),
        P("tp", None, None),
        P("tp", None, None),
        P("tp"),
        P("tp"),
        P("tp", "fs"),
        P(),
        P("fs", "tp"),
        P("fs", "tp"),
        P(None, "tp"),
        P(None, "tp"),
        P("tp", "fs"),
    )

    def body(*args):
        return local(mesh.shape["fs"], *args)

    return jax.shard_map(
        body,
        mesh=mesh,
        in_specs=placed,
        out_specs=P(("rep", "fs"), None, "tp"),
        check_vma=False,
    )
```

```python
import functools

import jax
import jax.numpy as jnp
import numpy as np
from jax import lax
from jax.experimental import pallas as pl
from jax.experimental.pallas import tpu as pltpu
from jax.sharding import PartitionSpec as P


EPS = 1e-06
GATE_SCALE = 8.0
TILE = 16
PARTS = 2
BLOCK_ROWS = 768
NORM_UNROLL = 8
SCAN_UNROLL = 3
ACT_UNROLL = 4
F32 = jnp.float32
BF16 = jnp.bfloat16


VMEM = pl.BlockSpec(memory_space=pltpu.VMEM)
SMEM = pl.BlockSpec(memory_space=pltpu.SMEM)
HBM = pl.BlockSpec(memory_space=pltpu.HBM)


def row_block(length):
    return max(b for b in range(TILE, BLOCK_ROWS + 1, TILE) if length % b == 0)


def fetch_rows(order_ref, pieces, wbuf, sems):
    rows = pieces[0].shape[0]
    copies = []
    for k, piece in enumerate(pieces):
        at = pl.multiple_of(order_ref[k] * rows, rows)
        copies.append(pltpu.make_async_copy(piece, wbuf.at[pl.ds(at, rows)], sems.at[k]))
    return copies


def fetch_blocks(order_ref, pieces, wbuf, sems, first=0):
    blocks = wbuf.shape[0]
    per = blocks // len(pieces)
    rows = pieces[0].shape[0] // per
    copies = []
    for k in range(blocks):
        source = pieces[k % len(pieces)].at[pl.ds(k // len(pieces) * rows, rows)]
        copies.append(pltpu.make_async_copy(source, wbuf.at[order_ref[k], pl.ds(0, rows)], sems.at[first + k]))
    return copies


def norm_into(own_ref, peer_ref, gain_ref, normed_ref):
    length, half = own_ref.shape

    def step(i, _):
        at = pl.ds(pl.multiple_of(i * TILE, TILE), TILE)
        own = own_ref[at, :].astype(F32)
        peer = peer_ref[at, :].astype(F32)
        mean_sq = jnp.sum(own * own + peer * peer, axis=1, keepdims=True) * (0.5 / half)
        scale = lax.rsqrt(mean_sq + EPS)
        normed_ref[at, :half] = (own * scale * gain_ref[0:1, :]).astype(BF16)
        normed_ref[at, half:] = (peer * scale * gain_ref[1:2, :]).astype(BF16)
        return 0

    lax.fori_loop(0, length // TILE, step, 0, unroll=NORM_UNROLL)


def fetch_streams(sources, buffers, sems, first):
    copies = []
    for k, (source, buffer) in enumerate(zip(sources, buffers)):
        rows = buffer.shape[0]
        part = source.at[pl.ds(source.shape[0] - rows, rows)]
        copies.append(pltpu.make_async_copy(part, buffer, sems.at[first + k]))
    return copies


def mix_kernel(n_pieces, order_ref, gain_ref, taps_ref, gates_ref, slope_ref, out_gain_ref, *rest):
    n_pieces -= 2
    streams, pieces = rest[:2], rest[2 : n_pieces + 2]
    mixed_ref, own_ref, peer_ref, normed_ref, wbuf, linear_ref, branch_ref, filt_ref, gate_ref, sems = rest[
        n_pieces + 2 :
    ]
    stream_copies = fetch_streams(streams, (own_ref, peer_ref), sems, n_pieces)
    copies = fetch_rows(order_ref, pieces, wbuf, sems)
    for copy in stream_copies + copies:
        copy.start()
    for copy in stream_copies:
        copy.wait()
    length, width = mixed_ref.shape
    block_count, block, _ = gates_ref.shape
    taps = taps_ref.shape[0]
    norm_into(own_ref, peer_ref, gain_ref, normed_ref)
    for copy in copies:
        copy.wait()
    linear_ref[0:8, :] = jnp.zeros((8, width), F32)
    rows = row_block(length)

    def project(m, _):
        at = pl.multiple_of(m * rows, rows)
        both = jnp.dot(normed_ref[pl.ds(at, rows), :], wbuf[...], preferred_element_type=F32).astype(BF16)
        linear_ref[pl.ds(pl.multiple_of(at + 8, 8), rows), :] = both[:, :width].astype(F32)
        branch_ref[pl.ds(at, rows), :] = both[:, width:]
        return 0

    lax.fori_loop(0, length // rows, project, 0)

    def convolve(i, _):
        at = pl.multiple_of(i * TILE, TILE)
        window = linear_ref[pl.ds(at, TILE + 8), :]
        total = window[9 - taps : 9 - taps + TILE] * taps_ref[0:1, :]
        for j in range(1, taps):
            total = total + window[9 - taps + j : 9 - taps + j + TILE] * taps_ref[j : j + 1, :]
        filt_ref[pl.ds(at, TILE), :] = total
        return 0

    lax.fori_loop(0, length // TILE, convolve, 0, unroll=2)

    def gates(m, _):
        at = pl.ds(pl.multiple_of(m * rows, rows), rows)
        for b in range(block_count):
            piece = filt_ref[at, b * block : (b + 1) * block].astype(BF16)
            gate_ref[at, 2 * b * block : 2 * (b + 1) * block] = jnp.dot(
                piece, gates_ref[b], preferred_element_type=F32
            )
        return 0

    lax.fori_loop(0, length // rows, gates, 0)
    row = lax.broadcasted_iota(jnp.int32, (8, block), 0)

    def scan(i, carry):
        at = pl.ds(pl.multiple_of(i * TILE, TILE), TILE)
        ends = []
        for b in range(block_count):
            cols = slice(b * block, (b + 1) * block)
            filtered = filt_ref[at, cols]
            rate = jax.nn.sigmoid(gate_ref[at, 2 * b * block : (2 * b + 1) * block])
            admit = jax.nn.sigmoid(gate_ref[at, (2 * b + 1) * block : 2 * (b + 1) * block])
            log_decay = rate * slope_ref[0:1, cols]
            fall = 1.0 / 120 + log_decay * (1.0 / 720)
            for coef in (1.0 / 24, 1.0 / 6, 0.5, 1.0):
                fall = coef + log_decay * fall
            fall = log_decay * fall
            decay = 1.0 + fall
            driven = jnp.sqrt(-fall * (2.0 + fall)) * admit * filtered
            last = carry[b]
            states = []
            for part in range(TILE // 8):
                a = decay[part * 8 : part * 8 + 8]
                d = driven[part * 8 : part * 8 + 8]
                for shift in (1, 2, 4):
                    keep = row >= shift
                    d = jnp.where(keep, a * pltpu.roll(d, shift, 0) + d, d)
                    a = jnp.where(keep, a * pltpu.roll(a, shift, 0), a)
                h = a * last + d
                last = jnp.broadcast_to(h[7:8, :], (8, block))
                states.append(h)
            ends.append(last)
            x = branch_ref[at, cols].astype(F32)
            gelu = 0.5 * x * (1.0 + jnp.tanh(0.7978845608028654 * (x + 0.044715 * x * x * x)))
            gated = jnp.concatenate(states, axis=0) * gelu
            mean_sq = jnp.mean(gated * gated, axis=1, keepdims=True)
            mixed_ref[at, cols] = (gated * lax.rsqrt(mean_sq + EPS) * out_gain_ref[0:1, cols]).astype(BF16)
        return tuple(ends)

    zero = jnp.zeros((8, block), F32)
    lax.fori_loop(0, length // TILE, scan, (zero,) * block_count, unroll=SCAN_UNROLL)


def add_kernel(starts, *refs):
    out_ref = refs[-1]

    def step(i, _):
        at = pl.multiple_of(i * TILE, TILE)
        total = None
        for start, ref in zip(starts, refs):
            term = ref[pl.ds(pl.multiple_of(start + at, TILE), TILE), :].astype(F32)
            total = term if total is None else total + term
        out_ref[pl.ds(at, TILE), :] = total.astype(BF16)
        return 0

    lax.fori_loop(0, out_ref.shape[0] // TILE, step, 0, unroll=2)


def final_kernel(start, chained, *refs):
    terms = refs[:4]
    out_ref, buffer_ref, sem = refs[4 + chained :]
    add_kernel([0] * 4, *terms, buffer_ref)
    copy = pltpu.make_async_copy(buffer_ref, out_ref.at[pl.ds(start, buffer_ref.shape[0])], sem)
    copy.start()
    copy.wait()


def ffn_kernel(halo, chunks, parts, n_down, n_pieces, order_ref, gain_ref, taps_ref, *rest):
    if halo:
        before_ref, rest = rest[0], rest[1:]
    n_streams = 2 * chunks
    streams, pieces, downs = rest[:n_streams], rest[n_streams : n_pieces - n_down], rest[n_pieces - n_down : n_pieces]
    outs, after_ref = rest[n_pieces : n_pieces + 2 * parts], rest[n_pieces + 2 * parts]
    own_ref, peer_ref, normed_ref, wbuf, pre_ref, hidden_ref, down_ref, sems = rest[n_pieces + 2 * parts + 1 :]
    n_pieces -= n_streams + n_down
    buffers = []
    for k, stream in enumerate(streams):
        rows = stream.shape[0]
        buffers.append((own_ref, peer_ref)[k // chunks].at[pl.ds(k % chunks * rows, rows)])
    stream_copies = fetch_streams(streams, buffers, sems, n_pieces)
    copies = fetch_rows(order_ref, pieces, wbuf, sems)
    down_copies = fetch_blocks(order_ref, downs, down_ref, sems, n_pieces + n_streams)
    for copy in stream_copies + copies + down_copies:
        copy.start()
    clear_padding(downs, down_ref)
    for copy in stream_copies:
        copy.wait()
    length = own_ref.shape[0]
    width = wbuf.shape[1]
    taps = taps_ref.shape[0]
    whole = width // 256
    norm_into(own_ref, peer_ref, gain_ref, normed_ref)
    for copy in copies:
        copy.wait()
    rows = row_block(length)
    pre_ref[0:8, :] = before_ref[...] if halo else jnp.zeros((8, width), F32)
    low = lax.broadcasted_iota(jnp.int32, (TILE, 128), 1) < 64

    def project(m, _):
        at = pl.multiple_of(m * rows, rows)
        pre = jnp.dot(normed_ref[pl.ds(at, rows), :], wbuf[...], preferred_element_type=F32)
        pre_ref[8 : 8 + rows, :] = pre.astype(BF16).astype(F32)

        def activate(i, _):
            r = pl.multiple_of(i * TILE, TILE)

            def conv(col):
                cols = slice(col, col + 128)
                window = pre_ref[pl.ds(r, TILE + 8), cols]
                total = window[9 - taps : 9 - taps + TILE] * taps_ref[0:1, cols]
                for j in range(1, taps):
                    total = total + window[9 - taps + j : 9 - taps + j + TILE] * taps_ref[j : j + 1, cols]
                return total

            out = pl.ds(pl.multiple_of(at + r, TILE), TILE)
            for b in range(whole):
                hidden = jax.nn.silu(conv(b * 128)) * conv((whole + b) * 128)
                hidden_ref[out, b * 128 : (b + 1) * 128] = hidden.astype(BF16)
            if width % 256:
                both = conv(2 * whole * 128)
                hidden = jnp.where(low, jax.nn.silu(both) * pltpu.roll(both, 64, 1), 0.0)
                hidden_ref[out, whole * 128 : (whole + 1) * 128] = hidden.astype(BF16)
            return 0

        lax.fori_loop(0, rows // TILE, activate, 0, unroll=ACT_UNROLL)
        pre_ref[0:8, :] = pre_ref[rows : rows + 8, :]
        return 0

    lax.fori_loop(0, length // rows, project, 0)
    after_ref[...] = pre_ref[0:8, :]
    for copy in down_copies:
        copy.wait()
    multiply_out(hidden_ref, down_ref, outs[:parts], outs[parts:])


def clear_padding(pieces, wbuf):
    blocks, padded, width = wbuf.shape
    depth = pieces[0].shape[0] * len(pieces) // blocks
    if padded > depth:
        wbuf[:, depth:, :] = jnp.zeros((blocks, padded - depth, width), BF16)


def multiply_out(left_ref, wbuf, keeps, sends):
    blocks, _, width = wbuf.shape
    length = keeps[0].shape[0]
    rows = row_block(length)
    for part in range(len(keeps)):

        def step(m, _):
            at = pl.multiple_of(m * rows, rows)
            left = left_ref[pl.ds(pl.multiple_of(part * length + at, rows), rows), :]
            for j in range(blocks):
                total = jnp.dot(left, wbuf[j], preferred_element_type=F32).astype(BF16)
                target = (keeps if j < blocks // 2 else sends)[part]
                col = (j % (blocks // 2)) * width
                target[pl.ds(at, rows), col : col + width] = total
            return 0

        lax.fori_loop(0, length // rows, step, 0)


def out_kernel(parts, n_pieces, order_ref, left_ref, *rest):
    pieces = rest[:n_pieces]
    keeps, sends = rest[n_pieces : n_pieces + parts], rest[n_pieces + parts : n_pieces + 2 * parts]
    wbuf, sems = rest[n_pieces + 2 * parts :]
    copies = fetch_blocks(order_ref, pieces, wbuf, sems)
    for copy in copies:
        copy.start()
    clear_padding(pieces, wbuf)
    for copy in copies:
        copy.wait()
    multiply_out(left_ref, wbuf, keeps, sends)


def call(kernel, outs, scratch, limit_mib, flops, operands, pieces, copies=None):
    specs = [SMEM] + [VMEM] * (len(operands) - 1) + [HBM] * len(pieces)
    return pl.pallas_call(
        functools.partial(kernel, len(pieces)),
        out_shape=outs,
        in_specs=specs,
        out_specs=jax.tree.map(lambda _: VMEM, outs),
        scratch_shapes=scratch + [pltpu.SemaphoreType.DMA((copies or len(pieces),))],
        compiler_params=pltpu.CompilerParams(vmem_limit_bytes=limit_mib * 1024 * 1024),
        cost_estimate=pl.CostEstimate(flops=flops, bytes_accessed=2**22, transcendentals=0),
    )(*operands, *pieces)


def line_ring(n):
    return [0] + list(range(1, n, 2)) + [i for i in range(n - 1, 0, -1) if i % 2 == 0]


def piece_table(n_fs):
    outer = n_fs // 2
    ring = line_ring(outer)
    table = np.zeros((n_fs, 2, n_fs), np.int32)
    for f in range(n_fs):
        z, y = divmod(f, 2)
        found = [ring[(ring.index(z) - k) % outer] for k in range(outer)]
        owners = [q * 2 + y for q in found] + [q * 2 + 1 - y for q in found]
        for c in range(2):
            for k, owner in enumerate(owners):
                half, inside = divmod(owner, n_fs // 2)
                table[f, c, k] = (half ^ c) * (n_fs // 2) + inside
    return table.reshape(n_fs * 2, n_fs)


def local(
    n_fs,
    stream_in,
    mix_gain,
    lin_weight,
    branch_weight,
    lin_taps,
    rate_blocks,
    admit_blocks,
    decay_logit,
    mix_out_gain,
    out_weight,
    ffn_gain,
    gate_weight,
    up_weight,
    gate_taps,
    up_taps,
    down_weight,
):
    outer = n_fs // 2
    ring = line_ring(outer)
    ring_pairs = [
        (ring[p] * 2 + y, ring[(p + 1) % outer] * 2 + y) for p in range(outer) for y in range(2)
    ]
    back_pairs = [(b, a) for a, b in ring_pairs]
    swap_pairs = [(f, f ^ 1) for f in range(n_fs)]
    flip = [(0, 1), (1, 0)]

    def across(value):
        return lax.ppermute(value, "rep", flip)

    def partner(value):
        return lax.ppermute(value, "tp", flip)

    def around(own, ahead=outer - 1):
        found = {0: own}
        for k in range(1, ahead + 1):
            found[k] = lax.ppermute(found[k - 1], "fs", ring_pairs)
        for k in range(outer - 1, ahead, -1):
            found[k] = lax.ppermute(found[(k + 1) % outer], "fs", back_pairs)
        return [found[k] for k in range(outer)]

    def gather_z_first(own, ahead=outer - 1):
        found = around(own, ahead)
        return found + [lax.ppermute(q, "fs", swap_pairs) for q in found]

    def gather_y_first(own):
        return around(jnp.concatenate([own, lax.ppermute(own, "fs", swap_pairs)], axis=0))

    x = lax.axis_index("rep")
    c = lax.axis_index("tp")
    f = lax.axis_index("fs")
    order = jnp.asarray(piece_table(n_fs))[f * 2 + c]

    def half_of(value, axis):
        size = value.shape[axis] // 2
        return lax.dynamic_slice_in_dim(value, x * size, size, axis)

    own = stream_in[0]
    length, half = own.shape
    part = length // PARTS
    channels = lin_weight.shape[1] // 2
    units = gate_weight.shape[1] // 2
    full = units // 128 * 128

    def interleave(gate, up):
        gate, up = half_of(gate, 1), half_of(up, 1)
        return jnp.concatenate([gate[:, :full], up[:, :full], gate[:, full:], up[:, full:]], axis=1)

    both = jnp.concatenate([half_of(lin_weight, 1), half_of(branch_weight, 1)], axis=1)
    mix_pieces = gather_z_first(both)
    other = across(own)
    own_peer = partner(own)
    other_peer = partner(other)
    out_pieces = gather_z_first(half_of(out_weight, 0))
    both = interleave(gate_weight, up_weight)
    ffn_pieces = gather_z_first(both)
    down_pieces = gather_y_first(half_of(down_weight, 0))

    gates = jnp.concatenate([half_of(rate_blocks, 0), half_of(admit_blocks, 0)], axis=2)
    slope = -GATE_SCALE * jax.nn.softplus(-half_of(decay_logit, 0))[None]
    out_gain = half_of(mix_out_gain, 0)[None]
    taps = half_of(lin_taps, 1)
    gain = jnp.where(c == 0, mix_gain.reshape(2, half), mix_gain.reshape(2, half)[::-1])
    gain2 = jnp.where(c == 0, ffn_gain.reshape(2, half), ffn_gain.reshape(2, half)[::-1])
    ffn_taps = interleave(gate_taps, up_taps)
    padded_units = -(-units // 128) * 128

    def mix(stream, peer):
        return call(
            mix_kernel,
            jax.ShapeDtypeStruct((length, channels), BF16),
            [
                pltpu.VMEM((length, half), BF16),
                pltpu.VMEM((length, half), BF16),
                pltpu.VMEM((length, 2 * half), BF16),
                pltpu.VMEM((2 * half, 2 * channels), BF16),
                pltpu.VMEM((length + 8, channels), F32),
                pltpu.VMEM((length, channels), BF16),
                pltpu.VMEM((length, channels), F32),
                pltpu.VMEM((length, 2 * channels), F32),
            ],
            30,
            length * 2 * half * 2 * channels * 2,
            [order, gain, taps, gates, slope, out_gain],
            [stream, peer] + mix_pieces,
        )

    def project(left, pieces):
        rows, depth = left.shape
        parts = rows // part
        sums = [jax.ShapeDtypeStruct((part, half), BF16)] * (2 * parts)
        outs = call(
            functools.partial(out_kernel, parts),
            sums,
            [pltpu.VMEM((n_fs, depth, pieces[0].shape[1]), BF16)],
            16,
            rows * depth * 2 * half * 2,
            [order, left],
            pieces,
            n_fs,
        )
        return outs[:parts], outs[parts:]

    def ffn(owns, peers, before):
        width = 2 * units
        parts = len(owns)
        rows = parts * part
        halo = [] if before is None else [before]
        pieces = owns + peers + ffn_pieces + down_pieces
        sums = [jax.ShapeDtypeStruct((part, half), BF16)] * (2 * parts)
        outs = call(
            functools.partial(ffn_kernel, bool(halo), parts, parts, len(down_pieces)),
            sums + [jax.ShapeDtypeStruct((8, width), F32)],
            [
                pltpu.VMEM((rows, half), BF16),
                pltpu.VMEM((rows, half), BF16),
                pltpu.VMEM((rows, 2 * half), BF16),
                pltpu.VMEM((2 * half, width), BF16),
                pltpu.VMEM((row_block(rows) + 8, width), F32),
                pltpu.VMEM((rows, padded_units), BF16),
                pltpu.VMEM((n_fs, padded_units, down_pieces[0].shape[1]), BF16),
            ],
            36,
            rows * 2 * half * width * 3,
            [order, gain2, ffn_taps] + halo,
            pieces,
            len(pieces) + n_fs,
        )
        return outs[:parts], outs[parts : 2 * parts], outs[2 * parts]

    def add(*terms):
        starts = [t[1] if isinstance(t, tuple) else 0 for t in terms]
        arrays = [t[0] if isinstance(t, tuple) else t for t in terms]
        return pl.pallas_call(
            functools.partial(add_kernel, starts),
            out_shape=jax.ShapeDtypeStruct((part, half), BF16),
            in_specs=[VMEM] * len(arrays),
            out_specs=VMEM,
            compiler_params=pltpu.CompilerParams(vmem_limit_bytes=12 * 1024 * 1024),
            cost_estimate=pl.CostEstimate(flops=part * half * len(arrays), bytes_accessed=2**21, transcendentals=0),
        )(*arrays)

    mixed_other = mix(other, other_peer)
    keep_other, send_other = project(mixed_other, out_pieces)
    sent = []
    for i in range(PARTS):
        value = add(keep_other[i], partner(send_other[i]))
        sent.append(across(value))
    mixed_own = mix(own, own_peer)
    keep_own, send_own = project(mixed_own, out_pieces)
    middle, middle_peer, middle_other = [], [], []
    for i in range(PARTS):
        value = add((own, i * part), keep_own[i], partner(send_own[i]), sent[i])
        middle.append(value)
        middle_other.append(across(value))
        middle_peer.append(partner(value))
    other_middle_peer = [partner(value) for value in middle_other]

    tail, sent = None, []
    for i in range(PARTS):
        keep, send, tail = ffn([middle_other[i]], [other_middle_peer[i]], tail)
        sent.append(across(add(keep[0], partner(send[0]))))
    keeps, sends, _ = ffn(middle, middle_peer, None)
    result = []
    for i in range(PARTS):
        terms = [middle[i], keeps[i], partner(sends[i]), sent[i]]
        run = pl.pallas_call(
            functools.partial(final_kernel, i * part, len(result)),
            out_shape=jax.ShapeDtypeStruct((length, half), BF16),
            in_specs=[VMEM] * 4 + [HBM] * len(result),
            out_specs=HBM,
            scratch_shapes=[pltpu.VMEM((part, half), BF16), pltpu.SemaphoreType.DMA],
            input_output_aliases={4: 0} if result else {},
            compiler_params=pltpu.CompilerParams(vmem_limit_bytes=12 * 1024 * 1024),
            cost_estimate=pl.CostEstimate(flops=part * half * 4, bytes_accessed=2**21, transcendentals=0),
        )
        result = [run(*terms, *result)]
    return result[0][None]


def solution(mesh):
    placed = (
        P(("rep", "fs"), None, "tp"),
        P(),
        P("fs", "tp"),
        P("fs", "tp"),
        P(None, "tp"),
        P("tp", None, None),
        P("tp", None, None),
        P("tp"),
        P("tp"),
        P("tp", "fs"),
        P(),
        P("fs", "tp"),
        P("fs", "tp"),
        P(None, "tp"),
        P(None, "tp"),
        P("tp", "fs"),
    )

    def body(*args):
        return local(mesh.shape["fs"], *args)

    return jax.shard_map(
        body,
        mesh=mesh,
        in_specs=placed,
        out_specs=P(("rep", "fs"), None, "tp"),
        check_vma=False,
    )
```

```python
import functools

import jax
import jax.numpy as jnp
import numpy as np
from jax import lax
from jax.experimental import pallas as pl
from jax.experimental.pallas import tpu as pltpu
from jax.sharding import PartitionSpec as P


EPS = 1e-06
GATE_SCALE = 8.0
TILE = 16
PARTS = 2
BLOCK_ROWS = 768
NORM_UNROLL = 8
SCAN_UNROLL = 3
ACT_UNROLL = 4
F32 = jnp.float32
BF16 = jnp.bfloat16


VMEM = pl.BlockSpec(memory_space=pltpu.VMEM)
SMEM = pl.BlockSpec(memory_space=pltpu.SMEM)
HBM = pl.BlockSpec(memory_space=pltpu.HBM)


def row_block(length):
    return max(b for b in range(TILE, BLOCK_ROWS + 1, TILE) if length % b == 0)


def fetch_rows(order_ref, pieces, wbuf, sems):
    rows = pieces[0].shape[0]
    copies = []
    for k, piece in enumerate(pieces):
        at = pl.multiple_of(order_ref[k] * rows, rows)
        copies.append(pltpu.make_async_copy(piece, wbuf.at[pl.ds(at, rows)], sems.at[k]))
    return copies


def fetch_blocks(order_ref, pieces, wbuf, sems, first=0):
    blocks = wbuf.shape[0]
    per = blocks // len(pieces)
    rows = pieces[0].shape[0] // per
    copies = []
    for k in range(blocks):
        source = pieces[k % len(pieces)].at[pl.ds(k // len(pieces) * rows, rows)]
        copies.append(pltpu.make_async_copy(source, wbuf.at[order_ref[k], pl.ds(0, rows)], sems.at[first + k]))
    return copies


def norm_into(own_ref, peer_ref, gain_ref, normed_ref):
    length, half = own_ref.shape

    def step(i, _):
        at = pl.ds(pl.multiple_of(i * TILE, TILE), TILE)
        own = own_ref[at, :].astype(F32)
        peer = peer_ref[at, :].astype(F32)
        mean_sq = jnp.sum(own * own + peer * peer, axis=1, keepdims=True) * (0.5 / half)
        scale = lax.rsqrt(mean_sq + EPS)
        normed_ref[at, :half] = (own * scale * gain_ref[0:1, :]).astype(BF16)
        normed_ref[at, half:] = (peer * scale * gain_ref[1:2, :]).astype(BF16)
        return 0

    lax.fori_loop(0, length // TILE, step, 0, unroll=NORM_UNROLL)


def fetch_streams(sources, buffers, sems, first):
    copies = []
    for k, (source, buffer) in enumerate(zip(sources, buffers)):
        rows = buffer.shape[0]
        part = source.at[pl.ds(source.shape[0] - rows, rows)]
        copies.append(pltpu.make_async_copy(part, buffer, sems.at[first + k]))
    return copies


def mix_kernel(n_pieces, order_ref, gain_ref, taps_ref, gates_ref, slope_ref, out_gain_ref, *rest):
    n_pieces -= 2
    streams, pieces = rest[:2], rest[2 : n_pieces + 2]
    mixed_ref, own_ref, peer_ref, normed_ref, wbuf, linear_ref, branch_ref, filt_ref, gate_ref, sems = rest[
        n_pieces + 2 :
    ]
    stream_copies = fetch_streams(streams, (own_ref, peer_ref), sems, n_pieces)
    copies = fetch_rows(order_ref, pieces, wbuf, sems)
    for copy in stream_copies + copies:
        copy.start()
    for copy in stream_copies:
        copy.wait()
    length, width = mixed_ref.shape
    block_count, block, _ = gates_ref.shape
    taps = taps_ref.shape[0]
    norm_into(own_ref, peer_ref, gain_ref, normed_ref)
    for copy in copies:
        copy.wait()
    linear_ref[0:8, :] = jnp.zeros((8, width), F32)
    rows = row_block(length)

    def project(m, _):
        at = pl.multiple_of(m * rows, rows)
        both = jnp.dot(normed_ref[pl.ds(at, rows), :], wbuf[...], preferred_element_type=F32).astype(BF16)
        linear_ref[pl.ds(pl.multiple_of(at + 8, 8), rows), :] = both[:, :width].astype(F32)
        branch_ref[pl.ds(at, rows), :] = both[:, width:]
        return 0

    lax.fori_loop(0, length // rows, project, 0)

    def convolve(i, _):
        at = pl.multiple_of(i * TILE, TILE)
        window = linear_ref[pl.ds(at, TILE + 8), :]
        total = window[9 - taps : 9 - taps + TILE] * taps_ref[0:1, :]
        for j in range(1, taps):
            total = total + window[9 - taps + j : 9 - taps + j + TILE] * taps_ref[j : j + 1, :]
        filt_ref[pl.ds(at, TILE), :] = total
        return 0

    lax.fori_loop(0, length // TILE, convolve, 0, unroll=2)

    def gates(m, _):
        at = pl.ds(pl.multiple_of(m * rows, rows), rows)
        for b in range(block_count):
            piece = filt_ref[at, b * block : (b + 1) * block].astype(BF16)
            gate_ref[at, 2 * b * block : 2 * (b + 1) * block] = jnp.dot(
                piece, gates_ref[b], preferred_element_type=F32
            )
        return 0

    lax.fori_loop(0, length // rows, gates, 0)
    row = lax.broadcasted_iota(jnp.int32, (8, block), 0)

    def scan(i, carry):
        at = pl.ds(pl.multiple_of(i * TILE, TILE), TILE)
        ends = []
        for b in range(block_count):
            cols = slice(b * block, (b + 1) * block)
            filtered = filt_ref[at, cols]
            rate = jax.nn.sigmoid(gate_ref[at, 2 * b * block : (2 * b + 1) * block])
            admit = jax.nn.sigmoid(gate_ref[at, (2 * b + 1) * block : 2 * (b + 1) * block])
            log_decay = rate * slope_ref[0:1, cols]
            fall = 1.0 / 120 + log_decay * (1.0 / 720)
            for coef in (1.0 / 24, 1.0 / 6, 0.5, 1.0):
                fall = coef + log_decay * fall
            fall = log_decay * fall
            decay = 1.0 + fall
            driven = jnp.sqrt(-fall * (2.0 + fall)) * admit * filtered
            last = carry[b]
            states = []
            for part in range(TILE // 8):
                a = decay[part * 8 : part * 8 + 8]
                d = driven[part * 8 : part * 8 + 8]
                for shift in (1, 2, 4):
                    keep = row >= shift
                    d = jnp.where(keep, a * pltpu.roll(d, shift, 0) + d, d)
                    a = jnp.where(keep, a * pltpu.roll(a, shift, 0), a)
                h = a * last + d
                last = jnp.broadcast_to(h[7:8, :], (8, block))
                states.append(h)
            ends.append(last)
            x = branch_ref[at, cols].astype(F32)
            gelu = 0.5 * x * (1.0 + jnp.tanh(0.7978845608028654 * (x + 0.044715 * x * x * x)))
            gated = jnp.concatenate(states, axis=0) * gelu
            mean_sq = jnp.mean(gated * gated, axis=1, keepdims=True)
            mixed_ref[at, cols] = (gated * lax.rsqrt(mean_sq + EPS) * out_gain_ref[0:1, cols]).astype(BF16)
        return tuple(ends)

    zero = jnp.zeros((8, block), F32)
    lax.fori_loop(0, length // TILE, scan, (zero,) * block_count, unroll=SCAN_UNROLL)


def add_kernel(starts, *refs):
    out_ref = refs[-1]

    def step(i, _):
        at = pl.multiple_of(i * TILE, TILE)
        total = None
        for start, ref in zip(starts, refs):
            term = ref[pl.ds(pl.multiple_of(start + at, TILE), TILE), :].astype(F32)
            total = term if total is None else total + term
        out_ref[pl.ds(at, TILE), :] = total.astype(out_ref.dtype)
        return 0

    lax.fori_loop(0, out_ref.shape[0] // TILE, step, 0, unroll=4)


def final_kernel(start, chained, *refs):
    out_ref, buffer_ref, sem = refs[2 + chained :]
    add_kernel([0] * 2, *refs[:2], buffer_ref)
    copy = pltpu.make_async_copy(buffer_ref, out_ref.at[pl.ds(start, buffer_ref.shape[0])], sem)
    copy.start()
    copy.wait()


def ffn_kernel(halo, chunks, parts, n_down, n_pieces, order_ref, gain_ref, taps_ref, *rest):
    if halo:
        before_ref, rest = rest[0], rest[1:]
    n_streams = 2 * chunks
    streams, pieces, downs = rest[:n_streams], rest[n_streams : n_pieces - n_down], rest[n_pieces - n_down : n_pieces]
    outs, after_ref = rest[n_pieces : n_pieces + 2 * parts], rest[n_pieces + 2 * parts]
    own_ref, peer_ref, normed_ref, wbuf, pre_ref, hidden_ref, down_ref, sems = rest[n_pieces + 2 * parts + 1 :]
    n_pieces -= n_streams + n_down
    buffers = []
    for k, stream in enumerate(streams):
        rows = stream.shape[0]
        buffers.append((own_ref, peer_ref)[k // chunks].at[pl.ds(k % chunks * rows, rows)])
    stream_copies = fetch_streams(streams, buffers, sems, n_pieces)
    copies = fetch_rows(order_ref, pieces, wbuf, sems)
    down_copies = fetch_blocks(order_ref, downs, down_ref, sems, n_pieces + n_streams)
    for copy in stream_copies + copies:
        copy.start()
    clear_padding(downs, down_ref)
    for copy in stream_copies:
        copy.wait()
    length = own_ref.shape[0]
    width = wbuf.shape[1]
    taps = taps_ref.shape[0]
    whole = width // 256
    norm_into(own_ref, peer_ref, gain_ref, normed_ref)
    for copy in copies:
        copy.wait()
    for copy in down_copies:
        copy.start()
    rows = row_block(length)
    pre_ref[0:8, :] = before_ref[...] if halo else jnp.zeros((8, width), F32)
    low = lax.broadcasted_iota(jnp.int32, (TILE, 128), 1) < 64

    def project(m, _):
        at = pl.multiple_of(m * rows, rows)
        pre = jnp.dot(normed_ref[pl.ds(at, rows), :], wbuf[...], preferred_element_type=F32)
        pre_ref[8 : 8 + rows, :] = pre.astype(BF16).astype(F32)

        def activate(i, _):
            r = pl.multiple_of(i * TILE, TILE)

            def conv(col):
                cols = slice(col, col + 128)
                window = pre_ref[pl.ds(r, TILE + 8), cols]
                total = window[9 - taps : 9 - taps + TILE] * taps_ref[0:1, cols]
                for j in range(1, taps):
                    total = total + window[9 - taps + j : 9 - taps + j + TILE] * taps_ref[j : j + 1, cols]
                return total

            out = pl.ds(pl.multiple_of(at + r, TILE), TILE)
            for b in range(whole):
                hidden = jax.nn.silu(conv(b * 128)) * conv((whole + b) * 128)
                hidden_ref[out, b * 128 : (b + 1) * 128] = hidden.astype(BF16)
            if width % 256:
                both = conv(2 * whole * 128)
                hidden = jnp.where(low, jax.nn.silu(both) * pltpu.roll(both, 64, 1), 0.0)
                hidden_ref[out, whole * 128 : (whole + 1) * 128] = hidden.astype(BF16)
            return 0

        lax.fori_loop(0, rows // TILE, activate, 0, unroll=ACT_UNROLL)
        pre_ref[0:8, :] = pre_ref[rows : rows + 8, :]
        return 0

    lax.fori_loop(0, length // rows, project, 0)
    after_ref[...] = pre_ref[0:8, :]
    for copy in down_copies:
        copy.wait()
    multiply_out(hidden_ref, down_ref, outs[:parts], outs[parts:])


def clear_padding(pieces, wbuf):
    blocks, padded, width = wbuf.shape
    depth = pieces[0].shape[0] * len(pieces) // blocks
    if padded > depth:
        wbuf[:, depth:, :] = jnp.zeros((blocks, padded - depth, width), BF16)


def multiply_out(left_ref, wbuf, keeps, sends):
    blocks, _, width = wbuf.shape
    length = keeps[0].shape[0]
    rows = row_block(length)
    for part in range(len(keeps)):

        def step(m, _):
            at = pl.multiple_of(m * rows, rows)
            left = left_ref[pl.ds(pl.multiple_of(part * length + at, rows), rows), :]
            for j in range(blocks):
                total = jnp.dot(left, wbuf[j], preferred_element_type=F32).astype(BF16)
                target = (keeps if j < blocks // 2 else sends)[part]
                col = (j % (blocks // 2)) * width
                target[pl.ds(at, rows), col : col + width] = total
            return 0

        lax.fori_loop(0, length // rows, step, 0)


def out_kernel(parts, n_pieces, order_ref, left_ref, *rest):
    pieces = rest[:n_pieces]
    keeps, sends = rest[n_pieces : n_pieces + parts], rest[n_pieces + parts : n_pieces + 2 * parts]
    wbuf, sems = rest[n_pieces + 2 * parts :]
    copies = fetch_blocks(order_ref, pieces, wbuf, sems)
    for copy in copies:
        copy.start()
    clear_padding(pieces, wbuf)
    for copy in copies:
        copy.wait()
    multiply_out(left_ref, wbuf, keeps, sends)


def call(kernel, outs, scratch, limit_mib, flops, operands, pieces, copies=None):
    specs = [SMEM] + [VMEM] * (len(operands) - 1) + [HBM] * len(pieces)
    return pl.pallas_call(
        functools.partial(kernel, len(pieces)),
        out_shape=outs,
        in_specs=specs,
        out_specs=jax.tree.map(lambda _: VMEM, outs),
        scratch_shapes=scratch + [pltpu.SemaphoreType.DMA((copies or len(pieces),))],
        compiler_params=pltpu.CompilerParams(vmem_limit_bytes=limit_mib * 1024 * 1024),
        cost_estimate=pl.CostEstimate(flops=flops, bytes_accessed=2**22, transcendentals=0),
    )(*operands, *pieces)


def line_ring(n):
    return [0] + list(range(1, n, 2)) + [i for i in range(n - 1, 0, -1) if i % 2 == 0]


def piece_table(n_fs):
    outer = n_fs // 2
    ring = line_ring(outer)
    table = np.zeros((n_fs, 2, n_fs), np.int32)
    for f in range(n_fs):
        z, y = divmod(f, 2)
        found = [ring[(ring.index(z) - k) % outer] for k in range(outer)]
        owners = [q * 2 + y for q in found] + [q * 2 + 1 - y for q in found]
        for c in range(2):
            for k, owner in enumerate(owners):
                half, inside = divmod(owner, n_fs // 2)
                table[f, c, k] = (half ^ c) * (n_fs // 2) + inside
    return table.reshape(n_fs * 2, n_fs)


def local(
    n_fs,
    stream_in,
    mix_gain,
    lin_weight,
    branch_weight,
    lin_taps,
    rate_blocks,
    admit_blocks,
    decay_logit,
    mix_out_gain,
    out_weight,
    ffn_gain,
    gate_weight,
    up_weight,
    gate_taps,
    up_taps,
    down_weight,
):
    outer = n_fs // 2
    ring = line_ring(outer)
    ring_pairs = [
        (ring[p] * 2 + y, ring[(p + 1) % outer] * 2 + y) for p in range(outer) for y in range(2)
    ]
    back_pairs = [(b, a) for a, b in ring_pairs]
    swap_pairs = [(f, f ^ 1) for f in range(n_fs)]
    flip = [(0, 1), (1, 0)]

    def across(value):
        return lax.ppermute(value, "rep", flip)

    def partner(value):
        return lax.ppermute(value, "tp", flip)

    def around(own, ahead=outer - 1):
        found = {0: own}
        for k in range(1, ahead + 1):
            found[k] = lax.ppermute(found[k - 1], "fs", ring_pairs)
        for k in range(outer - 1, ahead, -1):
            found[k] = lax.ppermute(found[(k + 1) % outer], "fs", back_pairs)
        return [found[k] for k in range(outer)]

    def gather_z_first(own, ahead=outer - 1):
        found = around(own, ahead)
        return found + [lax.ppermute(q, "fs", swap_pairs) for q in found]

    def gather_y_first(own):
        return around(jnp.concatenate([own, lax.ppermute(own, "fs", swap_pairs)], axis=0))

    x = lax.axis_index("rep")
    c = lax.axis_index("tp")
    f = lax.axis_index("fs")
    order = jnp.asarray(piece_table(n_fs))[f * 2 + c]

    def half_of(value, axis):
        size = value.shape[axis] // 2
        return lax.dynamic_slice_in_dim(value, x * size, size, axis)

    own = stream_in[0]
    length, half = own.shape
    part = length // PARTS
    channels = lin_weight.shape[1] // 2
    units = gate_weight.shape[1] // 2
    full = units // 128 * 128

    def interleave(gate, up):
        gate, up = half_of(gate, 1), half_of(up, 1)
        return jnp.concatenate([gate[:, :full], up[:, :full], gate[:, full:], up[:, full:]], axis=1)

    both = jnp.concatenate([half_of(lin_weight, 1), half_of(branch_weight, 1)], axis=1)
    mix_pieces = gather_z_first(both)
    other = across(own)
    own_peer = partner(own)
    other_peer = partner(other)
    out_pieces = gather_z_first(half_of(out_weight, 0))
    both = interleave(gate_weight, up_weight)
    ffn_pieces = gather_z_first(both)
    down_pieces = [
        pltpu.with_memory_space_constraint(piece, pltpu.HBM)
        for piece in gather_y_first(half_of(down_weight, 0))
    ]

    gates = jnp.concatenate([half_of(rate_blocks, 0), half_of(admit_blocks, 0)], axis=2)
    slope = -GATE_SCALE * jax.nn.softplus(-half_of(decay_logit, 0))[None]
    out_gain = half_of(mix_out_gain, 0)[None]
    taps = half_of(lin_taps, 1)
    gain = jnp.where(c == 0, mix_gain.reshape(2, half), mix_gain.reshape(2, half)[::-1])
    gain2 = jnp.where(c == 0, ffn_gain.reshape(2, half), ffn_gain.reshape(2, half)[::-1])
    ffn_taps = interleave(gate_taps, up_taps)
    padded_units = -(-units // 128) * 128

    def mix(stream, peer):
        return call(
            mix_kernel,
            jax.ShapeDtypeStruct((length, channels), BF16),
            [
                pltpu.VMEM((length, half), BF16),
                pltpu.VMEM((length, half), BF16),
                pltpu.VMEM((length, 2 * half), BF16),
                pltpu.VMEM((2 * half, 2 * channels), BF16),
                pltpu.VMEM((length + 8, channels), F32),
                pltpu.VMEM((length, channels), BF16),
                pltpu.VMEM((length, channels), F32),
                pltpu.VMEM((length, 2 * channels), F32),
            ],
            22,
            length * 2 * half * 2 * channels * 2,
            [order, gain, taps, gates, slope, out_gain],
            [stream, peer] + mix_pieces,
        )

    def project(left, pieces):
        rows, depth = left.shape
        parts = rows // part
        sums = [jax.ShapeDtypeStruct((part, half), BF16)] * (2 * parts)
        outs = call(
            functools.partial(out_kernel, parts),
            sums,
            [pltpu.VMEM((n_fs, depth, pieces[0].shape[1]), BF16)],
            10,
            rows * depth * 2 * half * 2,
            [order, left],
            pieces,
            n_fs,
        )
        return outs[:parts], outs[parts:]

    def ffn(owns, peers, before):
        width = 2 * units
        parts = len(owns)
        rows = parts * part
        halo = [] if before is None else [before]
        pieces = owns + peers + ffn_pieces + down_pieces
        sums = [jax.ShapeDtypeStruct((part, half), BF16)] * (2 * parts)
        outs = call(
            functools.partial(ffn_kernel, bool(halo), parts, parts, len(down_pieces)),
            sums + [jax.ShapeDtypeStruct((8, width), F32)],
            [
                pltpu.VMEM((rows, half), BF16),
                pltpu.VMEM((rows, half), BF16),
                pltpu.VMEM((rows, 2 * half), BF16),
                pltpu.VMEM((2 * half, width), BF16),
                pltpu.VMEM((row_block(rows) + 8, width), F32),
                pltpu.VMEM((rows, padded_units), BF16),
                pltpu.VMEM((n_fs, padded_units, down_pieces[0].shape[1]), BF16),
            ],
            20 if parts == 1 else 28,
            rows * 2 * half * width * 3,
            [order, gain2, ffn_taps] + halo,
            pieces,
            len(pieces) + n_fs,
        )
        return outs[:parts], outs[parts : 2 * parts], outs[2 * parts]

    def add(*terms, dtype=BF16):
        starts = [t[1] if isinstance(t, tuple) else 0 for t in terms]
        arrays = [t[0] if isinstance(t, tuple) else t for t in terms]
        return pl.pallas_call(
            functools.partial(add_kernel, starts),
            out_shape=jax.ShapeDtypeStruct((part, half), dtype),
            in_specs=[VMEM] * len(arrays),
            out_specs=VMEM,
            compiler_params=pltpu.CompilerParams(vmem_limit_bytes=12 * 1024 * 1024),
            cost_estimate=pl.CostEstimate(flops=part * half * len(arrays), bytes_accessed=2**21, transcendentals=0),
        )(*arrays)

    mixed_other = mix(other, other_peer)
    keep_other, send_other = project(mixed_other, out_pieces)
    sent = []
    for i in range(PARTS):
        value = add(keep_other[i], partner(send_other[i]))
        sent.append(across(value))
    mixed_own = mix(own, own_peer)
    keep_own, send_own = project(mixed_own, out_pieces)
    middle, middle_peer, middle_other = [], [], []
    for i in range(PARTS):
        value = add((own, i * part), keep_own[i], partner(send_own[i]), sent[i])
        middle.append(value)
        middle_other.append(across(value))
        middle_peer.append(partner(value))
    other_middle_peer = [partner(value) for value in middle_other]

    tail, sent = None, []
    for i in range(PARTS):
        keep, send, tail = ffn([middle_other[i]], [other_middle_peer[i]], tail)
        sent.append(across(add(keep[0], partner(send[0]))))
    keeps, sends, _ = ffn(middle, middle_peer, None)
    result = []
    for i in range(PARTS):
        local_sum = add(middle[i], keeps[i], partner(sends[i]), dtype=F32)
        run = pl.pallas_call(
            functools.partial(final_kernel, i * part, len(result)),
            out_shape=jax.ShapeDtypeStruct((length, half), BF16),
            in_specs=[VMEM] * 2 + [HBM] * len(result),
            out_specs=HBM,
            scratch_shapes=[pltpu.VMEM((part, half), BF16), pltpu.SemaphoreType.DMA],
            input_output_aliases={2: 0} if result else {},
            compiler_params=pltpu.CompilerParams(vmem_limit_bytes=12 * 1024 * 1024),
            cost_estimate=pl.CostEstimate(flops=part * half * 4, bytes_accessed=2**21, transcendentals=0),
        )
        result = [run(local_sum, sent[i], *result)]
    return result[0][None]


def solution(mesh):
    placed = (
        P(("rep", "fs"), None, "tp"),
        P(),
        P("fs", "tp"),
        P("fs", "tp"),
        P(None, "tp"),
        P("tp", None, None),
        P("tp", None, None),
        P("tp"),
        P("tp"),
        P("tp", "fs"),
        P(),
        P("fs", "tp"),
        P("fs", "tp"),
        P(None, "tp"),
        P(None, "tp"),
        P("tp", "fs"),
    )

    def body(*args):
        return local(mesh.shape["fs"], *args)

    return jax.shard_map(
        body,
        mesh=mesh,
        in_specs=placed,
        out_specs=P(("rep", "fs"), None, "tp"),
        check_vma=False,
    )
```
